256 devices in a mesh: grp: 2 (over y), sp: 32 (over z, core), tp: 4 (over x).
Axes of the slice: x: 4, y: 2, z: 16, core: 2. Of those that a mesh axis runs over, the one named last changes fastest.
The devices are a block of a 4x16x16 slice.
Arguments:
- stream: bfloat16 [16384, 2048], P(('grp', 'sp'), 'tp'), parts along dimension 0, may hold values from -1.5 to 1.5
- layer_norm_gain: float32 [2, 2048], replicated, may hold values from 0.1 to 1.9
- convolution_in_weight: bfloat16 [2, 2048, 1536], P(None, 'sp', 'tp'), may hold values from -0.125 to 0.125
- gating_in_weight: bfloat16 [2, 2048, 1536], P(None, 'sp', 'tp'), may hold values from -0.125 to 0.125
- output_weight: bfloat16 [2, 1536, 2048], P(None, 'tp', 'sp'), may hold values from -0.15625 to 0.15625
- convolution_kernel_taps: float32 [2, 4, 1536], P(None, None, 'tp'), may hold values from -12 to 12
- recurrent_gate_blocks: bfloat16 [2, 2, 2, 12, 128, 128], P(None, None, None, 'tp'), may hold values from -0.5 to 0.5
- channel_decay_logit: float32 [2, 2, 1536], P(None, None, 'tp')
- position_decay_boost: float32 [2, 2, 16384], P(None, None, ('grp', 'sp')), parts along dimension 2, may hold values from -1.4 to 0, as said below
Outputs:
- new_stream: bfloat16 [16384, 2048], P(('grp', 'sp'), 'tp'), parts along dimension 0
The draws below stay inside these ranges and needn't reach their ends.
There are 2 independent parts, one for each index of `grp`. The reference program is written for one: setup_inputs(seed, part) draws one part's arguments, and reference() takes and returns one part's arrays. A program takes and returns all parts, laid end to end along the dimension named above; an argument that names none is the same for every part. Nothing has to cross between parts.
Inputs may be any that keep to these rules, and one draw needn't show every extreme that they name: `position_decay_boost`: zero at all but a few positions.
All inputs are finite; a program needn't handle non-finite values.
Results may differ from the reference program's by a relative error of at most 0.025.
Values may be sent and summed in bfloat16 or wider, within the bound.
A program may use at most 128 MiB of HBM per device.

```python
import jax
import jax.numpy as jnp
from jax import lax

D = 2048
LRU = 1536
BW = 128
LAYERS = 2
TOKENS = 8192
N_TP = 4


def draw_channel_decay_logit(key, part):
    key_pick, key_slow, key_fast = jax.random.split(jax.random.fold_in(key, 11), 3)
    shape = (LAYERS, 2, LRU)
    share = 0.5
    slow = jax.random.uniform(key_pick, shape, jnp.float32) < share
    slow_rate = jax.random.uniform(key_slow, shape, jnp.float32, 0.03, 0.1) / TOKENS
    fast_rate = jnp.exp(jax.random.uniform(key_fast, shape, jnp.float32, jnp.log(0.004), jnp.log(0.0125)))
    return -jnp.log(jnp.where(slow, slow_rate, fast_rate))


def draw_position_decay_boost(key, part):
    key_spot, key_loss = jax.random.split(jax.random.fold_in(key, 23), 2)
    spots = jax.random.randint(key_spot, (LAYERS, 2, 2), 0, TOKENS)
    losses = jnp.log(jax.random.uniform(key_loss, (LAYERS, 2, 2), jnp.float32, 0.5, 0.8))
    positions = jnp.arange(TOKENS)
    return jnp.sum(jnp.where(positions[None, None, None, :] == spots[..., None], losses[..., None], 0.0), axis=2)


def draw_convolution_kernel_taps(key, part):
    noise = jax.random.normal(jax.random.fold_in(key, 37), (LAYERS, 4, LRU), jnp.float32)
    spread = jnp.array([3.0, 1.0, 1.0, 1.0], jnp.float32)
    return jnp.clip(noise * spread[None, :, None], -12.0, 12.0)


def block_levels(stream_key, extent, pieces, low, top_value):
    def one(position, blocks):
        steps = jax.random.uniform(jax.random.fold_in(jax.random.fold_in(stream_key, 6), position), (blocks,), jnp.float32, low / len(pieces), top_value / len(pieces))
        return jnp.repeat(jnp.exp(steps), extent[position] // blocks).reshape((-1,) + (1,) * (len(extent) - position - 1))

    loudness = one(*pieces[0])
    for cut in pieces[1:]:
        loudness = loudness * one(*cut)
    return loudness


def centred(own_key, extent, deviation, reach, shards=(), kind=jnp.bfloat16):
    result = deviation * jax.random.normal(own_key, extent, jnp.float32)
    if shards:
        result = result * block_levels(own_key, extent, shards, -0.22, 0.18)
    return jnp.clip(result, -reach, reach).astype(kind)


def setup_inputs(seed: int = 0, part: int = 0) -> dict:
    key_of = jax.random.split(jax.random.key(seed), 10)
    own_keys = jax.random.split(jax.random.fold_in(key_of[9], part), 10)
    stream = centred(own_keys[0], (TOKENS, D), 0.25, 1.5, ((0, 32), (1, 4)))
    layer_norm_gain = jnp.clip(1.0 + 0.18 * jax.random.normal(key_of[1], (LAYERS, D), jnp.float32), 0.1, 1.9)
    convolution_in_weight = centred(key_of[2], (LAYERS, D, LRU), D ** -0.5, 0.125, ((1, 32), (2, 4)))
    gating_in_weight = centred(key_of[3], (LAYERS, D, LRU), D ** -0.5, 0.125, ((1, 32), (2, 4)))
    output_weight = centred(key_of[4], (LAYERS, LRU, D), LRU ** -0.5, 0.15625, ((1, 4), (2, 32)))
    convolution_kernel_taps = draw_convolution_kernel_taps(jax.random.fold_in(key_of[9], 71), part)
    recurrent_gate_blocks = centred(key_of[6], (LAYERS, 2, 2, LRU // BW, BW, BW), BW ** -0.5, 0.5, ((3, 4),))
    channel_decay_logit = draw_channel_decay_logit(jax.random.fold_in(key_of[9], 71), part)
    position_decay_boost = draw_position_decay_boost(jax.random.fold_in(jax.random.fold_in(key_of[9], part), 71), part)
    return {"stream": stream, "layer_norm_gain": layer_norm_gain, "convolution_in_weight": convolution_in_weight, "gating_in_weight": gating_in_weight, "output_weight": output_weight, "convolution_kernel_taps": convolution_kernel_taps, "recurrent_gate_blocks": recurrent_gate_blocks, "channel_decay_logit": channel_decay_logit, "position_decay_boost": position_decay_boost}


EPS = 1e-06
RECURRENT_WIDTH = 8.0

def rms_norm(values, gain_row):
    floats = values.astype(jnp.float32)
    inverse = lax.rsqrt(lax.optimization_barrier(jnp.mean(floats * floats, axis=-1, keepdims=True)) + EPS)
    return (floats * inverse * gain_row.astype(jnp.float32)).astype(jnp.bfloat16)

def combine_pairs(earlier, latter):
    return (earlier[0] * latter[0], latter[0] * earlier[1] + latter[1])

def linear_recurrence(convolution_output, gate_matrix_pair, decay_logit_row, boost_row):
    seq_len = convolution_output.shape[0]
    block_width = gate_matrix_pair.shape[-1]
    conv_float = convolution_output.astype(jnp.float32)
    grouped = conv_float.reshape(seq_len, -1, block_width)
    recurrent_branch = jax.nn.sigmoid(jnp.einsum('tnc,ncd->tnd', grouped, gate_matrix_pair[0].astype(jnp.float32)).reshape(seq_len, -1))
    input_gate = jax.nn.sigmoid(jnp.einsum('tnc,ncd->tnd', grouped, gate_matrix_pair[1].astype(jnp.float32)).reshape(seq_len, -1))
    decay_logarithm = -RECURRENT_WIDTH * jax.nn.softplus(-decay_logit_row) * recurrent_branch + boost_row[:, None]
    is_start = (jnp.arange(seq_len) == 0)[:, None]
    multiplier = jnp.where(is_start, 1.0, jnp.sqrt(-jnp.expm1(2.0 * decay_logarithm)))
    driven = multiplier * input_gate * conv_float
    _, states = lax.associative_scan(combine_pairs, (jnp.exp(decay_logarithm), driven), axis=0)
    return states

def reference(stream, layer_norm_gain, convolution_in_weight, gating_in_weight, output_weight, convolution_kernel_taps, recurrent_gate_blocks, channel_decay_logit, position_decay_boost):
    seq_len = stream.shape[0]
    group_width = convolution_in_weight.shape[2] // N_TP
    for layer_index in range(LAYERS):
        normed = rms_norm(stream, layer_norm_gain[layer_index])
        proj_x = jnp.dot(normed, convolution_in_weight[layer_index], preferred_element_type=jnp.float32).astype(jnp.bfloat16)
        proj_y = jnp.dot(normed, gating_in_weight[layer_index], preferred_element_type=jnp.float32).astype(jnp.bfloat16)
        padded = jnp.pad(proj_x.astype(jnp.float32), ((1, 2), (0, 0)))
        taps_now = convolution_kernel_taps[layer_index]
        conv_mixed = taps_now[0] * padded[0:seq_len] + taps_now[1] * padded[1:seq_len + 1] + taps_now[2] * padded[2:seq_len + 2] + taps_now[3] * padded[3:seq_len + 3]
        convolution_output = conv_mixed.astype(jnp.bfloat16)
        forward_pass = linear_recurrence(convolution_output, recurrent_gate_blocks[layer_index, 0], channel_decay_logit[layer_index, 0], position_decay_boost[layer_index, 0])
        reverse_pass = jnp.flip(linear_recurrence(jnp.flip(convolution_output, 0), recurrent_gate_blocks[layer_index, 1], channel_decay_logit[layer_index, 1], jnp.flip(position_decay_boost[layer_index, 1], 0)), 0)
        gated = ((forward_pass + reverse_pass) * jax.nn.gelu(proj_y.astype(jnp.float32))).astype(jnp.bfloat16)
        branch = jnp.zeros((seq_len, stream.shape[1]), jnp.float32)
        for group in range(N_TP):
            lower = group * group_width
            partial_out = jnp.dot(gated[:, lower:lower + group_width], output_weight[layer_index, lower:lower + group_width, :], preferred_element_type=jnp.float32).astype(jnp.bfloat16)
            branch = branch + partial_out.astype(jnp.float32)
        stream = (stream.astype(jnp.float32) + branch).astype(jnp.bfloat16)
    return stream
```

```python
import functools

import jax
import jax.numpy as jnp
from jax import lax
from jax.experimental import pallas as pl
from jax.experimental.pallas import tpu as pltpu
from jax.sharding import PartitionSpec as P

EPS = 1e-06
RECURRENT_WIDTH = 8.0
SEG = 8
LAG = 3
CHUNKS = 2
F32 = jnp.float32
BF16 = jnp.bfloat16
MESH = pl.DeviceIdType.MESH


def dot(a, b):
    return jnp.dot(a, b, preferred_element_type=F32)


def dot_nt(a, b):
    return lax.dot_general(a, b, (((1,), (1,)), ((), ())), preferred_element_type=F32)


def dot_tn(a, b):
    return lax.dot_general(a, b, (((0,), (0,)), ((), ())), preferred_element_type=F32)


def one_minus_square(log_decay, decay):
    u = -2.0 * log_decay
    series = 1.0 - u * (1.0 / 6.0)
    for k in (5.0, 4.0, 3.0, 2.0):
        series = 1.0 - u * (1.0 / k) * series
    return jnp.where(u < 0.25, u * series, 1.0 - decay * decay)


def kernel(
    n_sp,
    n_tp,
    stream,
    gain,
    wx,
    wy,
    wo,
    taps,
    gates,
    logit,
    boost,
    out,
    wfull,
    feat,
    normed,
    px,
    halo_prev,
    halo_next,
    ext,
    conv,
    dec,
    drv,
    gel,
    mine,
    states,
    gated,
    part,
    relay_in,
    rs_left,
    rs_right,
    w_recv,
    w_send,
    pair_recv,
    ag_recv,
    ag_send,
    rs_recv,
    rs_send,
    halo_recv,
    halo_send,
    st_recv,
    st_send,
):
    layers = wx.shape[0]
    rows = stream.shape[0]
    cols = stream.shape[1]
    width = cols * n_tp
    shard = wx.shape[1]
    ch = wx.shape[2]
    block = gates.shape[-1]
    steps = rows // SEG
    mats = 3 * layers
    chips = n_sp // 2
    crow = rows // CHUNKS

    me = lax.axis_index("sp")
    x = lax.axis_index("tp")

    def sp_at(offset):
        return lax.rem(me + (offset + n_sp), n_sp)

    def tp_at(offset):
        return lax.rem(x + (offset + n_tp), n_tp)

    partner = me + 1 - 2 * lax.rem(me, 2)
    xr, xl, xo = tp_at(1), tp_at(-1), tp_at(2)

    def send(src, dst, ssem, rsem, **where):
        pltpu.make_async_remote_copy(
            src_ref=src,
            dst_ref=dst,
            send_sem=ssem,
            recv_sem=rsem,
            device_id=where,
            device_id_type=MESH,
        ).start()

    def landed(ref, sem):
        pltpu.make_async_copy(ref, ref, sem).wait()

    def own_rows(owner):
        return pl.ds(pl.multiple_of(owner * shard, shard), shard)

    def reach(m, d):
        far, near = chips // 2, chips - 1 - chips // 2
        return far if (m + d) % 2 == 0 else near

    def w_slot(m, owner):
        return wfull.at[m, own_rows(owner)]

    def hand_over(m, owner):
        send(w_slot(m, owner), w_slot(m, owner), w_send.at[m], pair_recv.at[m], sp=partner)

    def stage(t):
        for m in range(mats):
            k = t - LAG * m
            if k < 0 or k > chips // 2:
                continue
            for d in range(2):
                if k > reach(m, d):
                    continue
                owner = sp_at(-2 * k if d == 0 else 2 * k)
                if k > 0:
                    landed(w_slot(m, owner), w_hop(m, d, k))
                if k < reach(m, d):
                    send(
                        w_slot(m, owner),
                        w_slot(m, owner),
                        w_send.at[m],
                        w_hop(m, d, k + 1),
                        sp=sp_at(2 if d == 0 else -2),
                    )
                if k > 0 or d == 0:
                    hand_over(m, owner)

    def w_hop(m, d, k):
        return w_recv.at[m, d, k - 1]

    at = [0]
    stages = LAG * (mats - 1) + chips // 2 + 1

    def advance(upto):
        while at[0] <= min(upto, stages - 1):
            stage(at[0])
            at[0] += 1

    def complete(m):
        advance(LAG * m + chips // 2)
        landed(wfull.at[m, pl.ds(0, chips * shard)], pair_recv.at[m])

    def chunk(c):
        return pl.ds(c * crow, crow)

    def gather_send(l, c):
        own = feat.at[l, x, chunk(c)]
        send(own, own, ag_send.at[l], ag_recv.at[l, 0, c], tp=xr)
        send(own, own, ag_send.at[l], ag_recv.at[l, 1, c], tp=xl)

    def gather_relay(l, c):
        from_left = feat.at[l, xl, chunk(c)]
        from_right = feat.at[l, xr, chunk(c)]
        if c % 2 == 0:
            landed(from_left, ag_recv.at[l, 0, c])
            send(from_left, from_left, ag_send.at[l], ag_recv.at[l, 2, c], tp=xr)
            landed(from_right, ag_recv.at[l, 1, c])
        else:
            landed(from_right, ag_recv.at[l, 1, c])
            send(from_right, from_right, ag_send.at[l], ag_recv.at[l, 2, c], tp=xl)
            landed(from_left, ag_recv.at[l, 0, c])

    def gather_end(l, c):
        landed(feat.at[l, xo, chunk(c)], ag_recv.at[l, 2, c])

    barrier = pltpu.get_barrier_semaphore()
    for offset in (1, -1, 2, -2):
        pl.semaphore_signal(barrier, inc=1, device_id={"sp": sp_at(offset)}, device_id_type=MESH)
    for peer in (xr, xl):
        pl.semaphore_signal(barrier, inc=1, device_id={"tp": peer}, device_id_type=MESH)

    row_at = lax.broadcasted_iota(jnp.int32, (rows, rows), 0)
    col_at = lax.broadcasted_iota(jnp.int32, (rows, rows), 1)
    perm = (col_at == lax.rem(row_at, SEG) * steps + row_at // SEG).astype(BF16)
    eye = (
        lax.broadcasted_iota(jnp.int32, (shard, shard), 0)
        == lax.broadcasted_iota(jnp.int32, (shard, shard), 1)
    ).astype(BF16)
    for l in range(layers):
        wfull[3 * l, own_rows(me), :] = wx[l]
        wfull[3 * l + 1, own_rows(me), :] = wy[l]
        wfull[3 * l + 2, own_rows(me), :] = dot_nt(eye, wo[l]).astype(BF16)
    feat[0, x, :, :] = dot(perm, stream[...]).astype(BF16)

    pl.semaphore_wait(barrier, 6)
    advance(0)
    for c in range(CHUNKS):
        gather_send(0, c)

    boost_rows = jnp.concatenate(
        [boost[l, d : d + 1, :] for l in range(layers) for d in range(2)]
        + [jnp.zeros((8 - 2 * layers, rows), F32)],
        axis=0,
    )
    high = boost_rows.astype(BF16)
    rest = boost_rows - high.astype(F32)
    middle = rest.astype(BF16)
    low = (rest - middle.astype(F32)).astype(BF16)
    boost_cols = dot_nt(perm, high) + dot_nt(perm, middle) + dot_nt(perm, low)

    rate = -RECURRENT_WIDTH * jax.nn.softplus(-logit[...])

    advance(1)
    advance(2)
    for c in range(CHUNKS):
        gather_relay(0, c)

    sub = lax.broadcasted_iota(jnp.int32, (SEG, ch), 0)
    row_id = lax.broadcasted_iota(jnp.int32, (rows, 1), 0)

    for l in range(layers):
        if l == 0:
            complete(0)
        for c in range(CHUNKS):
            if l == 0:
                gather_end(l, c)
            total = None
            for o in range(n_tp):
                f = feat[l, o, chunk(c), :].astype(F32)
                s = jnp.sum(f * f, axis=1, keepdims=True)
                total = s if total is None else total + s
            inverse = lax.rsqrt(total * (1.0 / width) + EPS)
            for o in range(n_tp):
                f = feat[l, o, chunk(c), :].astype(F32)
                g = gain[l : l + 1, o * cols : (o + 1) * cols]
                normed[chunk(c), o * cols : (o + 1) * cols] = (f * inverse * g).astype(BF16)
        px_now = dot(normed[...], wfull[3 * l]).astype(BF16)
        px[l] = px_now
        send(px.at[l, pl.ds(0, 16)], halo_next.at[l], halo_send.at[l], halo_recv.at[l, 0], sp=sp_at(-1))
        send(
            px.at[l, pl.ds(rows - 16, 16)], halo_prev.at[l], halo_send.at[l], halo_recv.at[l, 1], sp=sp_at(1)
        )
        if l == 0:
            advance(9)
        else:
            complete(3 * l + 1)
            y = dot(normed[...], wfull[3 * l + 1]).astype(BF16).astype(F32)
            gel[...] = jax.nn.gelu(y)
        ext[SEG : SEG + rows, :] = px_now.astype(F32)
        landed(halo_next.at[l], halo_recv.at[l, 0])
        landed(halo_prev.at[l], halo_recv.at[l, 1])
        before = jnp.where(me > 0, halo_prev[l].astype(F32)[8:16], 0.0)
        after = jnp.where(me < n_sp - 1, halo_next[l].astype(F32), 0.0)
        ext[0:SEG, :] = jnp.where(
            sub == 0, pltpu.roll(before, 1, 0), pltpu.roll(ext[rows : rows + SEG, :], 1, 0)
        )
        for k in range(2):
            ext[SEG + rows + k * SEG : SEG + rows + (k + 1) * SEG, :] = jnp.where(
                sub == SEG - 1,
                pltpu.roll(after[k * SEG : (k + 1) * SEG], SEG - 1, 0),
                pltpu.roll(ext[SEG + k * SEG : SEG + (k + 1) * SEG, :], SEG - 1, 0),
            )
        mixed = taps[l, 0:1, :] * ext[0:rows, :]
        for k in range(1, 4):
            mixed = mixed + taps[l, k : k + 1, :] * ext[k * SEG : k * SEG + rows, :]
        conv[...] = mixed.astype(BF16)
        for b in range(ch // block):
            lanes = slice(b * block, (b + 1) * block)
            cv = conv[:, lanes]
            cvf = cv.astype(F32)
            for d in range(2):
                recur = jax.nn.sigmoid(dot(cv, gates[l, d, 0, b]))
                inject = jax.nn.sigmoid(dot(cv, gates[l, d, 1, b]))
                log_decay = (
                    rate[l, d : d + 1, lanes] * recur + boost_cols[:, 2 * l + d : 2 * l + d + 1]
                )
                decay = jnp.exp(log_decay)
                multiplier = jnp.sqrt(one_minus_square(log_decay, decay))
                if d == 0:
                    first = jnp.logical_and(row_id == 0, me == 0)
                else:
                    first = jnp.logical_and(row_id == rows - 1, me == n_sp - 1)
                multiplier = jnp.where(first, 1.0, multiplier)
                dec[d, :, lanes] = decay
                drv[d, :, lanes] = multiplier * inject * cvf
        if l == 0:
            advance(10)
        carry = [None, None]
        for j in range(steps):
            for d in range(2):
                q = j if d == 0 else steps - 1 - j
                r = slice(q * SEG, (q + 1) * SEG)
                a, h = dec[d, r, :], drv[d, r, :]
                if carry[d] is not None:
                    h = a * carry[d][1] + h
                    a = a * carry[d][0]
                    dec[d, r, :] = a
                    drv[d, r, :] = h
                carry[d] = (a, h)
        into = []
        for d in range(2):
            a, h = carry[d]
            for hop in (1, 2, 4):
                shift = hop if d == 0 else SEG - hop
                inside = sub >= hop if d == 0 else sub < SEG - hop
                a_far, h_far = pltpu.roll(a, shift, 0), pltpu.roll(h, shift, 0)
                h = jnp.where(inside, a * h_far + h, h)
                a = jnp.where(inside, a * a_far, a)
            end = SEG - 1 if d == 0 else 0
            mine[l, d, 0:1, :] = a[end : end + 1, :]
            mine[l, d, 1:2, :] = h[end : end + 1, :]
            shift = 1 if d == 0 else SEG - 1
            inside = sub >= 1 if d == 0 else sub < SEG - 1
            into.append(
                (
                    jnp.where(inside, pltpu.roll(a, shift, 0), 1.0),
                    jnp.where(inside, pltpu.roll(h, shift, 0), 0.0),
                )
            )
        order = sorted(range(1, n_sp), key=lambda o: -min(o, n_sp - o))
        for offset in order:
            wraps = jnp.where(me + offset >= n_sp, 1, 0)
            send(
                mine.at[l, wraps],
                states.at[l, me],
                st_send.at[l],
                st_recv.at[l],
                sp=sp_at(offset),
            )
        states[l, me, :, :] = mine[l, 0]
        if l == 0:
            complete(1)
            y = dot(normed[...], wfull[1]).astype(BF16).astype(F32)
            gel[...] = jax.nn.gelu(y)
            advance(12)
        landed(states.at[l, pl.ds(0, n_sp - 1)], st_recv.at[l])
        enter = []
        for d in range(2):
            e = jnp.zeros((1, ch), F32)
            for q in range(n_sp):
                k = q if d == 0 else n_sp - 1 - q
                take = me > k if d == 0 else me < k
                e = jnp.where(take, states[l, k, 0:1, :] * e + states[l, k, 1:2, :], e)
            enter.append(into[d][0] * e + into[d][1])
        for j in range(steps // 2):
            pieces = []
            for q in (2 * j, 2 * j + 1):
                r = slice(q * SEG, (q + 1) * SEG)
                s = (drv[0, r, :] + dec[0, r, :] * enter[0]) + (drv[1, r, :] + dec[1, r, :] * enter[1])
                pieces.append(s * gel[r, :])
            gated[2 * j * SEG : (2 * j + 2) * SEG, :] = jnp.concatenate(pieces, axis=0).astype(BF16)
        complete(3 * l + 2)

        def partial(dest, c):
            w = wfull[3 * l + 2, pl.ds(pl.multiple_of(dest * cols, cols), cols), :]
            part[l, dest, chunk(c), :] = dot_nt(gated[chunk(c), :], w).astype(BF16)

        def post(dest, c, to, ref, which):
            send(
                part.at[l, dest, chunk(c)],
                ref.at[l, chunk(c)],
                rs_send.at[l],
                rs_recv.at[l, which, c],
                tp=to,
            )

        for c in range(CHUNKS):
            ahead, behind = (xr, xl) if c % 2 == 0 else (xl, xr)
            partial(xo, c)
            post(xo, c, ahead, relay_in, 0)
            partial(behind, c)
            if c % 2 == 0:
                post(behind, c, behind, rs_right, 2)
            else:
                post(behind, c, behind, rs_left, 1)
            partial(ahead, c)
            partial(x, c)
        for c in range(CHUNKS):
            ahead = xr if c % 2 == 0 else xl
            landed(relay_in.at[l, chunk(c)], rs_recv.at[l, 0, c])
            both = part[l, ahead, chunk(c), :].astype(F32) + relay_in[l, chunk(c), :].astype(F32)
            part[l, ahead, chunk(c), :] = both.astype(BF16)
            if c % 2 == 0:
                post(ahead, c, ahead, rs_left, 1)
            else:
                post(ahead, c, ahead, rs_right, 2)
        if l == 0:
            advance(LAG * 3 + chips // 2 - 1)
        for c in range(CHUNKS):
            landed(rs_left.at[l, chunk(c)], rs_recv.at[l, 1, c])
            landed(rs_right.at[l, chunk(c)], rs_recv.at[l, 2, c])
            fresh = (
                feat[l, x, chunk(c), :].astype(F32)
                + part[l, x, chunk(c), :].astype(F32)
                + rs_left[l, chunk(c), :].astype(F32)
                + rs_right[l, chunk(c), :].astype(F32)
            ).astype(BF16)
            if l + 1 < layers:
                feat[l + 1, x, chunk(c), :] = fresh
                gather_send(l + 1, c)
            else:
                normed[chunk(c), 0:cols] = fresh
        if l + 1 < layers:
            for c in range(CHUNKS):
                gather_relay(l + 1, c)
            complete(3 * l + 3)
            for c in range(CHUNKS):
                gather_end(l + 1, c)

    out[...] = dot_tn(perm, normed[:, 0:cols]).astype(BF16)

    for m in range(mats):
        landed(wfull.at[m, pl.ds(0, (2 * chips - 1) * shard)], w_send.at[m])
    for l in range(layers):
        landed(feat.at[l, pl.ds(0, 3)], ag_send.at[l])
        landed(part.at[l, pl.ds(0, 3)], rs_send.at[l])
        landed(px.at[l, pl.ds(0, 32)], halo_send.at[l])
        landed(states.at[l, pl.ds(0, n_sp - 1)], st_send.at[l])


def local(n_sp, n_tp, stream, gain, wx, wy, wo, taps, gates, logit, boost):
    layers, shard, ch = wx.shape
    rows, cols = stream.shape
    width = cols * n_tp
    mats = 3 * layers
    vmem = pl.BlockSpec(memory_space=pltpu.VMEM)
    dma = pltpu.SemaphoreType.DMA
    return pl.pallas_call(
        functools.partial(kernel, n_sp, n_tp),
        out_shape=jax.ShapeDtypeStruct((rows, cols), BF16),
        in_specs=[vmem] * 9,
        out_specs=vmem,
        scratch_shapes=[
            pltpu.VMEM((mats, width, ch), BF16),
            pltpu.VMEM((layers, n_tp, rows, cols), BF16),
            pltpu.VMEM((rows, width), BF16),
            pltpu.VMEM((layers, rows, ch), BF16),
            pltpu.VMEM((layers, 16, ch), BF16),
            pltpu.VMEM((layers, 16, ch), BF16),
            pltpu.VMEM((rows + 3 * SEG, ch), F32),
            pltpu.VMEM((rows, ch), BF16),
            pltpu.VMEM((2, rows, ch), F32),
            pltpu.VMEM((2, rows, ch), F32),
            pltpu.VMEM((rows, ch), F32),
            pltpu.VMEM((layers, 2, 2, ch), F32),
            pltpu.VMEM((layers, n_sp, 2, ch), F32),
            pltpu.VMEM((rows, ch), BF16),
            pltpu.VMEM((layers, n_tp, rows, cols), BF16),
            pltpu.VMEM((layers, rows, cols), BF16),
            pltpu.VMEM((layers, rows, cols), BF16),
            pltpu.VMEM((layers, rows, cols), BF16),
            dma((mats, 2, n_sp // 4)),
            dma((mats,)),
            dma((mats,)),
            dma((layers, 3, CHUNKS)),
            dma((layers,)),
            dma((layers, 3, CHUNKS)),
            dma((layers,)),
            dma((layers, 2)),
            dma((layers,)),
            dma((layers,)),
            dma((layers,)),
        ],
        compiler_params=pltpu.CompilerParams(
            collective_id=0, has_side_effects=True, vmem_limit_bytes=56 * 1024 * 1024
        ),
        name="whole",
    )(stream, gain, wx, wy, wo, taps, gates, logit, boost)


def solution(mesh):
    return jax.shard_map(
        functools.partial(local, mesh.shape["sp"], mesh.shape["tp"]),
        mesh=mesh,
        in_specs=(
            P(("grp", "sp"), "tp"),
            P(),
            P(None, "sp", "tp"),
            P(None, "sp", "tp"),
            P(None, "tp", "sp"),
            P(None, None, "tp"),
            P(None, None, None, "tp", None, None),
            P(None, None, "tp"),
            P(None, None, ("grp", "sp")),
        ),
        out_specs=P(("grp", "sp"), "tp"),
        check_vma=False,
    )
```
